32 devices in a mesh: grp: 2 (over y), fs: 4 (over z), tp: 4 (over x, core).
Axes of the slice: x: 2, y: 2, z: 4, core: 2. Of those that a mesh axis runs over, the one named last changes fastest.
Arguments:
- residual_in: bfloat16 [4096, 2048], P(('grp', 'fs', 'tp')), parts along dimension 0, may hold values from -6 to 6
- hidden_first: bfloat16 [4096, 5632], P(('grp', 'fs', 'tp')), parts along dimension 0, may hold values from -6 to 6
- down_weight: bfloat16 [5632, 2048], P('tp', 'fs'), may hold values from -0.078125 to 0.078125
- mixer_out: bfloat16 [4096, 2048], P(('grp', 'fs', 'tp')), parts along dimension 0, may hold values from -6 to 6
- norm_gain: float32 [2, 2048], replicated, may hold values from 0.1 to 1.9
- norm_shift: float32 [2, 2048], replicated, may hold values from -1.5 to 1.5
- gate_weight: bfloat16 [2048, 5632], P('fs', 'tp'), may hold values from -0.125 to 0.125
- up_weight: bfloat16 [2048, 5632], P('fs', 'tp'), may hold values from -0.125 to 0.125
Outputs:
- mixed_state: bfloat16 [4096, 2048], P(('grp', 'fs', 'tp')), parts along dimension 0
- hidden_second: bfloat16 [4096, 5632], P(('grp', 'fs'), 'tp'), parts along dimension 0
The draws below stay inside these ranges and needn't reach their ends.
There are 2 independent parts, one for each index of `grp`. The reference program is written for one: setup_inputs(seed, part) draws one part's arguments, and reference() takes and returns one part's arrays. A program takes and returns all parts, laid end to end along the dimension named above; an argument that names none is the same for every part. Nothing has to cross between parts.
All inputs are finite; a program needn't handle non-finite values.
Results may differ from the reference program's by a relative error of at most 0.012.
Values may be sent and summed in bfloat16 or wider, within the bound.
A program may use at most 64 MiB of HBM per device.

```python
import jax
import jax.numpy as jnp
from jax import lax

D = 2048
FF = 5632
TOKENS = 2048
N_TP = 4


def block_scale(stream_key, dims, split, low, largest):
    loudness, own = 1.0, jax.random.fold_in(stream_key, 6)
    for position, shards_of in split:
        steps = jnp.exp(jax.random.uniform(jax.random.fold_in(own, position), (shards_of,), jnp.float32, low / len(split), largest / len(split)))
        loudness = loudness * jnp.repeat(steps, dims[position] // shards_of).reshape([-1 if axis == position else 1 for axis in range(len(dims))])
    return loudness


def normal_values(stream_key, dims, scale, bound, pieces=(), held_as=jnp.bfloat16):
    entries = scale * jax.random.normal(stream_key, dims, jnp.float32)
    if pieces:
        entries = entries * block_scale(stream_key, dims, pieces, -0.22, 0.18)
    return jnp.clip(entries, -bound, bound).astype(held_as)


def setup_inputs(seed: int = 0, part: int = 0) -> dict:
    key_of = jax.random.split(jax.random.key(seed), 9)
    part_keys = jax.random.split(jax.random.fold_in(key_of[8], part), 9)
    residual_in = normal_values(part_keys[0], (TOKENS, D), 1.0, 6.0, ((0, 16),))
    hidden_first = normal_values(part_keys[1], (TOKENS, FF), 1.0, 6.0, ((0, 16),))
    down_weight = normal_values(key_of[2], (FF, D), FF ** -0.5, 0.078125, ((0, 4), (1, 4)))
    mixer_out = normal_values(part_keys[3], (TOKENS, D), 1.0, 6.0, ((0, 16),))
    norm_gain = jnp.clip(1.0 + 0.18 * jax.random.normal(key_of[4], (2, D), jnp.float32), 0.1, 1.9)
    norm_shift = normal_values(key_of[5], (2, D), 0.3, 1.5, (), jnp.float32)
    gate_weight = normal_values(key_of[6], (D, FF), D ** -0.5, 0.125, ((0, 4), (1, 4)))
    up_weight = normal_values(key_of[7], (D, FF), D ** -0.5, 0.125, ((0, 4), (1, 4)))
    return dict(residual_in=residual_in, hidden_first=hidden_first, down_weight=down_weight, mixer_out=mixer_out, norm_gain=norm_gain, norm_shift=norm_shift, gate_weight=gate_weight, up_weight=up_weight)


def layer_norm(values, gain, shift):
    center = values - lax.optimization_barrier(jnp.mean(values, axis=-1, keepdims=True))
    variance = lax.optimization_barrier(jnp.mean(center * center, axis=-1, keepdims=True))
    return center * lax.rsqrt(variance + 1e-05) * gain + shift

def reference(residual_in, hidden_first, down_weight, mixer_out, norm_gain, norm_shift, gate_weight, up_weight):
    width = FF // N_TP

    def add_block(total, index):
        start = (index * width).astype(jnp.int32)
        rows = lax.dynamic_slice_in_dim(hidden_first, start, width, 1)
        cols = lax.dynamic_slice_in_dim(down_weight, start, width, 0)
        term = jnp.dot(rows, cols, preferred_element_type=jnp.float32).astype(jnp.bfloat16)
        term = lax.optimization_barrier(term)
        return (total + term.astype(jnp.float32), None)
    empty = jnp.zeros((hidden_first.shape[0], down_weight.shape[1]), jnp.float32)
    branch, _ = lax.scan(add_block, empty, jnp.arange(N_TP, dtype=jnp.int32))
    first = layer_norm(jnp.sqrt(2.0) * residual_in.astype(jnp.float32) + 0.5 * branch, norm_gain[0], norm_shift[0])
    mixed_state = layer_norm(jnp.sqrt(2.0) * first + mixer_out.astype(jnp.float32), norm_gain[1], norm_shift[1]).astype(jnp.bfloat16)
    gate = jnp.dot(mixed_state, gate_weight, preferred_element_type=jnp.float32)
    up = jnp.dot(mixed_state, up_weight, preferred_element_type=jnp.float32)
    hidden_second = (jax.nn.silu(gate) * up).astype(jnp.bfloat16)
    return (mixed_state, hidden_second)
```

```python
import functools

import jax
import jax.numpy as jnp
from jax import lax
from jax.experimental import pallas as pl
from jax.experimental.pallas import tpu as pltpu
from jax.sharding import PartitionSpec as P

MESH = pl.DeviceIdType.MESH


def layer_norm(values, gain, shift):
    center = values - jnp.mean(values, axis=-1, keepdims=True)
    variance = jnp.mean(center * center, axis=-1, keepdims=True)
    return center * lax.rsqrt(variance + 1e-05) * gain + shift


def kernel(
    sizes,
    res_ref,
    hid_ref,
    down_ref,
    mix_ref,
    gain_ref,
    shift_ref,
    gate_ref,
    up_ref,
    mixed_ref,
    out_ref,
    down_all,
    pair_all,
    spread,
    part,
    red,
    mixed_all,
    acc,
    load_sem,
    d_send,
    d_recv,
    w_send,
    w_recv,
    a_send,
    a_recv,
    r_send,
    r_recv,
    m_send,
    m_recv,
):
    n_grp, n_fs, n_tp, sub = sizes
    g, f, t = lax.axis_index("grp"), lax.axis_index("fs"), lax.axis_index("tp")
    rows = res_ref.shape[0]
    width = gate_ref.shape[1]
    depth = gate_ref.shape[0]
    cols = down_ref.shape[1]
    chunks = n_grp * sub
    d_rows = down_ref.shape[0] // chunks
    w_rows = depth // chunks

    def hid_block(peer):
        if len(hid_ref.shape) == 3:
            return hid_ref.at[peer]
        return hid_ref.at[:, pl.ds(pl.multiple_of(peer * width, width), width)]

    def own_rows(peer):
        return pl.ds(pl.multiple_of(peer * rows, rows), rows)

    load_down = pltpu.make_async_copy(down_ref, down_all.at[f], load_sem.at[0])
    load_gate = pltpu.make_async_copy(gate_ref, pair_all.at[f, 0], load_sem.at[1])
    load_up = pltpu.make_async_copy(up_ref, pair_all.at[f, 1], load_sem.at[2])
    load_hid = pltpu.make_async_copy(hid_block(t), spread.at[own_rows(t)], load_sem.at[3])
    load_down.start()
    load_hid.start()
    load_gate.start()
    load_up.start()

    barrier = pltpu.get_barrier_semaphore()

    def greet(device):
        pl.semaphore_signal(barrier, inc=1, device_id=device, device_id_type=MESH)

    for d in range(1, n_grp):
        greet({"grp": lax.rem(g + d, n_grp)})
    for d in range(1, n_tp):
        greet({"tp": lax.rem(t + d, n_tp)})

    @pl.when(f > 0)
    def _():
        greet({"fs": f - 1})

    @pl.when(f < n_fs - 1)
    def _():
        greet({"fs": f + 1})

    inner = jnp.minimum(f, 1) + jnp.minimum(n_fs - 1 - f, 1)
    pl.semaphore_wait(barrier, n_grp - 1 + n_tp - 1 + inner)

    def d_copy(src, chunk, way, device):
        block = down_all.at[src, pl.ds(pl.multiple_of(chunk * d_rows, d_rows), d_rows)]
        return pltpu.make_async_remote_copy(
            src_ref=block,
            dst_ref=block,
            send_sem=d_send.at[way, src, chunk],
            recv_sem=d_recv.at[src, chunk],
            device_id=device,
            device_id_type=MESH,
        )

    def w_copy(mat):
        def copy(src, chunk, way, device):
            block = pair_all.at[src, mat, pl.ds(pl.multiple_of(chunk * w_rows, w_rows), w_rows)]
            return pltpu.make_async_remote_copy(
                src_ref=block,
                dst_ref=block,
                send_sem=w_send.at[way, 2 * src + mat, chunk],
                recv_sem=w_recv.at[2 * src + mat, chunk],
                device_id=device,
                device_id_type=MESH,
            )

        return copy

    def along(copy, src, chunk, act):
        @pl.when((f < n_fs - 1) & (src <= f))
        def _():
            act(copy(src, chunk, 0, {"fs": f + 1}))

        @pl.when((f > 0) & (src >= f))
        def _():
            act(copy(src, chunk, 1, {"fs": f - 1}))

    def across(copy, src, chunk, act):
        for d in range(1, n_grp):
            act(copy(src, chunk, 1 + d, {"grp": lax.rem(g + d, n_grp)}))

    def start(copy):
        copy.start()

    def wait_send(copy):
        copy.wait_send()

    def take(copies, src):
        for j in range(sub):
            for copy in copies:
                chunk = g * sub + j
                copy(src, chunk, 0, {"fs": f}).wait_recv()
                along(copy, src, chunk, start)
                across(copy, src, chunk, start)

    def take_across(copies, src):
        for d in range(1, n_grp):
            peer = lax.rem(g + d, n_grp)
            for j in range(sub):
                for copy in copies:
                    copy(src, peer * sub + j, 0, {"fs": f}).wait_recv()

    def source(k):
        return f + (1 - 2 * lax.rem(k, 2)) * ((k + 1) // 2)

    def valid(src):
        return (src >= 0) & (src < n_fs)

    w_copies = [w_copy(0), w_copy(1)]

    def a_copy(d):
        peer = lax.rem(t + d, n_tp)
        return pltpu.make_async_remote_copy(
            src_ref=hid_block(peer),
            dst_ref=spread.at[own_rows(t)],
            send_sem=a_send.at[d],
            recv_sem=a_recv.at[d],
            device_id={"tp": peer},
            device_id_type=MESH,
        )

    def r_copy(src, d):
        peer = lax.rem(t + d, n_tp)
        return pltpu.make_async_remote_copy(
            src_ref=part.at[src, own_rows(peer)],
            dst_ref=red.at[d, src],
            send_sem=r_send.at[d, src],
            recv_sem=r_recv.at[d, src],
            device_id={"tp": peer},
            device_id_type=MESH,
        )

    def m_copy(d):
        peer = lax.rem(t + d, n_tp)
        return pltpu.make_async_remote_copy(
            src_ref=mixed_all.at[own_rows(t)],
            dst_ref=mixed_all.at[own_rows(t)],
            send_sem=m_send.at[d],
            recv_sem=m_recv.at[d],
            device_id={"tp": peer},
            device_id_type=MESH,
        )

    load_down.wait()
    for j in range(sub):
        along(d_copy, f, g * sub + j, start)
    for d in range(1, n_tp):
        a_copy(d).start()
    load_gate.wait()
    load_up.wait()
    load_hid.wait()

    def first_half(k, carry):
        src = source(k)

        @pl.when(valid(src))
        def _():
            take([d_copy], src)

        @pl.when(k == 2 * n_fs - 2)
        def _():
            for j in range(sub):
                for copy in w_copies:
                    along(copy, f, g * sub + j, start)

        @pl.when(k == 2)
        def _():
            for d in range(1, n_tp):
                a_copy(d).wait_recv()

        done = source(k - 2)

        @pl.when((k >= 2) & valid(done))
        def _():
            @pl.when(k > 2)
            def _():
                take_across([d_copy], done)

            part[done] = jnp.dot(
                spread[...], down_all[done], preferred_element_type=jnp.float32
            ).astype(jnp.bfloat16)
            for d in range(1, n_tp):
                r_copy(done, d).start()

        return carry

    lax.fori_loop(1, 2 * n_fs + 1, first_half, 0)

    for src in range(n_fs):
        for d in range(1, n_tp):
            r_copy(src, d).wait_recv()
    pieces = []
    for src in range(n_fs):
        total = part[src, own_rows(t)].astype(jnp.float32)
        for d in range(1, n_tp):
            total = total + red[d, src].astype(jnp.float32)
        pieces.append(total)
    branch = jnp.concatenate(pieces, axis=1)
    first = layer_norm(
        jnp.sqrt(2.0) * res_ref[...].astype(jnp.float32) + 0.5 * branch,
        gain_ref[0:1],
        shift_ref[0:1],
    )
    mixed = layer_norm(
        jnp.sqrt(2.0) * first + mix_ref[...].astype(jnp.float32), gain_ref[1:2], shift_ref[1:2]
    ).astype(jnp.bfloat16)
    mixed_all[own_rows(t)] = mixed
    mixed_ref[...] = mixed
    for d in range(1, n_tp):
        m_copy(d).start()
    acc[...] = jnp.zeros_like(acc)

    def second_half(k, carry):
        src = source(k)

        @pl.when(valid(src))
        def _():
            take(w_copies, src)

        @pl.when(k == 2)
        def _():
            for d in range(1, n_tp):
                m_copy(d).wait_recv()

        done = source(k - 2)

        @pl.when((k >= 2) & valid(done))
        def _():
            @pl.when(k > 2)
            def _():
                take_across(w_copies, done)

            here = pl.ds(pl.multiple_of(done * depth, depth), depth)
            for mat in range(2):
                acc[mat] += jnp.dot(
                    mixed_all[:, here], pair_all[done, mat], preferred_element_type=jnp.float32
                )

        return carry

    lax.fori_loop(1, 2 * n_fs + 1, second_half, 0)
    gate = acc[0]
    out_ref[...] = (gate / (1.0 + jnp.exp(-gate)) * acc[1]).astype(jnp.bfloat16)

    for d in range(1, n_tp):
        a_copy(d).wait_send()
        m_copy(d).wait_send()
        for src in range(n_fs):
            r_copy(src, d).wait_send()

    def drain(src, carry):
        for copy in [d_copy] + w_copies:
            for j in range(sub):
                along(copy, src, g * sub + j, wait_send)

                @pl.when(src != f)
                def _():
                    across(copy, src, g * sub + j, wait_send)

        return carry

    lax.fori_loop(0, n_fs, drain, 0)


def on_device(
    sizes,
    residual_in,
    hidden_first,
    down_weight,
    mixer_out,
    norm_gain,
    norm_shift,
    gate_weight,
    up_weight,
):
    n_grp, n_fs, n_tp = sizes
    rows, model = residual_in.shape
    depth, width = gate_weight.shape
    cols = down_weight.shape[1]
    sub = 1
    if depth % (n_grp * 2 * 32) == 0 and down_weight.shape[0] % (n_grp * 2 * 32) == 0:
        sub = 2
    chunks = n_grp * sub
    if width % 128:
        hidden_first = hidden_first.reshape(rows, n_tp, width).transpose(1, 0, 2)
    vmem = pl.BlockSpec(memory_space=pltpu.VMEM)
    anywhere = pl.BlockSpec(memory_space=pl.ANY)
    dma = pltpu.SemaphoreType.DMA
    tokens = rows * n_tp
    return pl.pallas_call(
        functools.partial(kernel, (n_grp, n_fs, n_tp, sub)),
        out_shape=(
            jax.ShapeDtypeStruct((rows, model), jnp.bfloat16),
            jax.ShapeDtypeStruct((tokens, width), jnp.bfloat16),
        ),
        in_specs=[vmem, anywhere, anywhere, vmem, vmem, vmem, anywhere, anywhere],
        out_specs=(vmem, vmem),
        scratch_shapes=[
            pltpu.VMEM((n_fs,) + down_weight.shape, jnp.bfloat16),
            pltpu.VMEM((n_fs, 2, depth, width), jnp.bfloat16),
            pltpu.VMEM((tokens, width), jnp.bfloat16),
            pltpu.VMEM((n_fs, tokens, cols), jnp.bfloat16),
            pltpu.VMEM((n_tp, n_fs, rows, cols), jnp.bfloat16),
            pltpu.VMEM((tokens, model), jnp.bfloat16),
            pltpu.VMEM((2, tokens, width), jnp.float32),
            dma((4,)),
            dma((1 + n_grp, n_fs, chunks)),
            dma((n_fs, chunks)),
            dma((1 + n_grp, 2 * n_fs, chunks)),
            dma((2 * n_fs, chunks)),
            dma((n_tp,)),
            dma((n_tp,)),
            dma((n_tp, n_fs)),
            dma((n_tp, n_fs)),
            dma((n_tp,)),
            dma((n_tp,)),
        ],
        compiler_params=pltpu.CompilerParams(
            collective_id=0, has_side_effects=True, vmem_limit_bytes=60 * 1024 * 1024
        ),
        name="half_steps",
    )(
        residual_in,
        hidden_first,
        down_weight,
        mixer_out,
        norm_gain,
        norm_shift,
        gate_weight,
        up_weight,
    )


def solution(mesh):
    sizes = tuple(mesh.shape[axis] for axis in ("grp", "fs", "tp"))
    in_specs = (
        P(("grp", "fs", "tp"), None),
        P(("grp", "fs", "tp"), None),
        P("tp", "fs"),
        P(("grp", "fs", "tp"), None),
        P(),
        P(),
        P("fs", "tp"),
        P("fs", "tp"),
    )
    out_specs = (P(("grp", "fs", "tp"), None), P(("grp", "fs"), "tp"))
    return jax.shard_map(
        functools.partial(on_device, sizes),
        mesh=mesh,
        in_specs=in_specs,
        out_specs=out_specs,
        check_vma=False,
    )
```

```python
import functools

import jax
import jax.numpy as jnp
from jax import lax
from jax.experimental import pallas as pl
from jax.experimental.pallas import tpu as pltpu
from jax.sharding import PartitionSpec as P

MESH = pl.DeviceIdType.MESH


def layer_norm(values, gain, shift):
    center = values - jnp.mean(values, axis=-1, keepdims=True)
    variance = jnp.mean(center * center, axis=-1, keepdims=True)
    return center * lax.rsqrt(variance + 1e-05) * gain + shift


def kernel(
    sizes,
    res_ref,
    hid_ref,
    down_ref,
    mix_ref,
    gain_ref,
    shift_ref,
    gate_ref,
    up_ref,
    mixed_ref,
    out_ref,
    down_all,
    host_all,
    each_all,
    spread,
    part,
    red,
    mixed_all,
    host_acc,
    each_acc,
    back,
    load_sem,
    d_send,
    d_recv,
    h_send,
    h_recv,
    e_send,
    e_recv,
    a_send,
    a_recv,
    r_send,
    r_recv,
    m_send,
    m_recv,
    g_send,
    g_recv,
    b_send,
    b_recv,
):
    n_grp, n_fs, n_tp, sub = sizes
    shared = host_all.shape[3]
    g, f, t = lax.axis_index("grp"), lax.axis_index("fs"), lax.axis_index("tp")
    rows = res_ref.shape[0]
    width = gate_ref.shape[1]
    depth = gate_ref.shape[0]
    chunks = n_grp * sub

    def hid_block(peer):
        if len(hid_ref.shape) == 3:
            return hid_ref.at[peer]
        return hid_ref.at[:, pl.ds(pl.multiple_of(peer * width, width), width)]

    def own_rows(peer):
        return pl.ds(pl.multiple_of(peer * rows, rows), rows)

    load_down = pltpu.make_async_copy(down_ref, down_all.at[f], load_sem.at[0])
    loads = []
    for mat, ref in enumerate((gate_ref, up_ref)):
        loads.append(
            pltpu.make_async_copy(
                ref.at[:, pl.ds(0, shared)], host_all.at[f, mat], load_sem.at[1 + mat]
            )
        )
        loads.append(
            pltpu.make_async_copy(
                ref.at[:, pl.ds(shared, width - shared)], each_all.at[f, mat], load_sem.at[4 + mat]
            )
        )
    load_hid = pltpu.make_async_copy(hid_block(t), spread.at[own_rows(t)], load_sem.at[3])
    load_down.start()
    load_hid.start()
    for load in loads:
        load.start()

    lower = 2 * (f // 2)
    half = n_fs // 2
    host = lower + jnp.where(lower + 1 < half, 1, 0)
    is_host = f == host
    other = 2 * lower + 1 - f
    low_host = 1 if half > 1 else 0
    high_host = 2 * ((n_fs - 1) // 2)

    barrier = pltpu.get_barrier_semaphore()

    def greet(device):
        pl.semaphore_signal(barrier, inc=1, device_id=device, device_id_type=MESH)

    for d in range(1, n_grp):
        greet({"grp": lax.rem(g + d, n_grp)})
    for d in range(1, n_tp):
        greet({"tp": lax.rem(t + d, n_tp)})

    @pl.when(f > 0)
    def _():
        greet({"fs": f - 1})

    @pl.when(f < n_fs - 1)
    def _():
        greet({"fs": f + 1})

    inner = jnp.minimum(f, 1) + jnp.minimum(n_fs - 1 - f, 1)
    pl.semaphore_wait(barrier, n_grp - 1 + n_tp - 1 + inner)

    def block_copy(all_refs, send, recv):
        def copy(src, chunk, way, device):
            blocks = all_refs(src)
            size = blocks.shape[0] // chunks
            block = blocks.at[pl.ds(pl.multiple_of(chunk * size, size), size)]
            return pltpu.make_async_remote_copy(
                src_ref=block,
                dst_ref=block,
                send_sem=send(src).at[way, chunk],
                recv_sem=recv(src).at[chunk],
                device_id=device,
                device_id_type=MESH,
            )

        return copy

    def weight(refs, send, recv, mat):
        return block_copy(
            lambda src: refs.at[src, mat],
            lambda src: send.at[2 * src + mat],
            lambda src: recv.at[2 * src + mat],
        )

    def start(copy):
        copy.start()

    def wait_send(copy):
        copy.wait_send()

    class Gather:
        def __init__(self, copies, low, high, whole, needs):
            self.copies, self.low, self.high = copies, low, high
            self.whole, self.needs = whole, needs

        def whole_up(self, plane):
            return (2 * plane < n_fs) & self.whole

        def whole_down(self, plane):
            return (2 * plane >= n_fs) & self.whole

        def reached(self, plane):
            return (plane >= self.low) & (plane <= self.high)

        def along(self, copy, src, chunk, act, mine):
            up = (src <= f) & self.reached(f + 1)
            down = (src >= f) & self.reached(f - 1)
            if not mine:
                up = up & self.whole_up(f + 1)
                down = down & self.whole_down(f - 1)

            @pl.when(up)
            def _():
                act(copy(src, chunk, 0, {"fs": f + 1}))

            @pl.when(down)
            def _():
                act(copy(src, chunk, 1, {"fs": f - 1}))

        def all_along(self, src, act):
            for j in range(sub):
                for copy in self.copies:
                    self.along(copy, src, g * sub + j, act, True)
            if self.whole:
                for d in range(1, n_grp):
                    for j in range(sub):
                        for copy in self.copies:
                            chunk = lax.rem(g + d, n_grp) * sub + j
                            self.along(copy, src, chunk, act, False)

        def across(self, copy, src, chunk, act):
            for d in range(1, n_grp):
                act(copy(src, chunk, 1 + d, {"grp": lax.rem(g + d, n_grp)}))

        def whole_in(self, src):
            return ((src < f) & self.whole_up(f)) | ((src > f) & self.whole_down(f))

        def comes(self, src):
            return (src >= 0) & (src < n_fs) & (src != f) & self.reached(f)

        def swaps(self, src):
            return self.comes(src) & self.needs & jnp.logical_not(self.whole_in(src))

        def take(self, src):
            @pl.when(self.comes(src))
            def _():
                for j in range(sub):
                    for copy in self.copies:
                        chunk = g * sub + j
                        copy(src, chunk, 0, {"fs": other}).wait_recv()
                        self.along(copy, src, chunk, start, True)

                        @pl.when(self.swaps(src))
                        def _():
                            self.across(copy, src, chunk, start)

            if self.whole:

                @pl.when(self.comes(src) & self.whole_in(src))
                def _():
                    for d in range(1, n_grp):
                        for j in range(sub):
                            for copy in self.copies:
                                chunk = lax.rem(g + d, n_grp) * sub + j
                                copy(src, chunk, 0, {"fs": other}).wait_recv()
                                self.along(copy, src, chunk, start, False)

        def take_across(self, src):
            @pl.when(self.swaps(src))
            def _():
                for d in range(1, n_grp):
                    for j in range(sub):
                        for copy in self.copies:
                            chunk = lax.rem(g + d, n_grp) * sub + j
                            copy(src, chunk, 0, {"fs": other}).wait_recv()

        def drain(self, src):
            @pl.when((src == f) | self.comes(src))
            def _():
                if self.whole:
                    @pl.when((src == f) | self.whole_in(src))
                    def _():
                        for d in range(1, n_grp):
                            for j in range(sub):
                                for copy in self.copies:
                                    chunk = lax.rem(g + d, n_grp) * sub + j
                                    self.along(copy, src, chunk, wait_send, False)
                for j in range(sub):
                    for copy in self.copies:
                        self.along(copy, src, g * sub + j, wait_send, True)

            @pl.when(self.swaps(src))
            def _():
                for j in range(sub):
                    for copy in self.copies:
                        self.across(copy, src, g * sub + j, wait_send)

    def source(k):
        return f + (1 - 2 * lax.rem(k, 2)) * ((k + 1) // 2)

    def valid(src):
        return (src >= 0) & (src < n_fs)

    d_copy = block_copy(
        lambda src: down_all.at[src], lambda src: d_send.at[src], lambda src: d_recv.at[src]
    )
    down = Gather([d_copy], 0, n_fs - 1, False, True)
    hosted = Gather(
        [weight(host_all, h_send, h_recv, mat) for mat in range(2)],
        low_host,
        high_host,
        True,
        is_host,
    )
    each = Gather(
        [weight(each_all, e_send, e_recv, mat) for mat in range(2)], 0, n_fs - 1, True, True
    )

    def a_copy(d):
        peer = lax.rem(t + d, n_tp)
        return pltpu.make_async_remote_copy(
            src_ref=hid_block(peer),
            dst_ref=spread.at[own_rows(t)],
            send_sem=a_send.at[d],
            recv_sem=a_recv.at[d],
            device_id={"tp": peer},
            device_id_type=MESH,
        )

    def r_copy(src, d):
        peer = lax.rem(t + d, n_tp)
        return pltpu.make_async_remote_copy(
            src_ref=part.at[src, own_rows(peer)],
            dst_ref=red.at[d, src],
            send_sem=r_send.at[d, src],
            recv_sem=r_recv.at[d, src],
            device_id={"tp": peer},
            device_id_type=MESH,
        )

    core = lax.rem(t, 2)
    sibling = t + 1 - 2 * core

    def m_copy(owner, whose, hop):
        peer = sibling if hop == 0 else lax.rem(t + 2 * hop, n_tp)
        place = mixed_all.at[whose, own_rows(owner)]
        return pltpu.make_async_remote_copy(
            src_ref=place,
            dst_ref=place,
            send_sem=m_send.at[whose, owner, hop],
            recv_sem=m_recv.at[whose, owner],
            device_id={"tp": peer},
            device_id_type=MESH,
        )

    chips = n_tp // 2

    def m_out(whose):
        for hop in list(range(1, chips)) + [0]:
            m_copy(t, whose, hop).start()

    def m_relay(whose):
        for hop in range(1, chips):
            owner = lax.rem(t + 2 * hop, n_tp)
            m_copy(owner, whose, 0).wait_recv()
            m_copy(owner, whose, 0).start()

    def m_rest(whose):
        for hop in range(chips):
            m_copy(lax.rem(sibling + 2 * hop, n_tp), whose, 0).wait_recv()

    def m_drain(whose):
        for hop in range(chips):
            m_copy(t, whose, hop).wait_send()
        for hop in range(1, chips):
            m_copy(lax.rem(t + 2 * hop, n_tp), whose, 0).wait_send()

    def g_copy():
        return pltpu.make_async_remote_copy(
            src_ref=mixed_all.at[0, own_rows(t)],
            dst_ref=mixed_all.at[1, own_rows(t)],
            send_sem=g_send.at[0],
            recv_sem=g_recv.at[0],
            device_id={"fs": other},
            device_id_type=MESH,
        )

    tiles = 2
    tile = n_tp * rows // tiles

    def tile_rows(i):
        return pl.ds(pl.multiple_of(i * tile, tile), tile)

    def b_copy(i):
        return pltpu.make_async_remote_copy(
            src_ref=back.at[tile_rows(i)],
            dst_ref=out_ref.at[tile_rows(i), pl.ds(0, shared)],
            send_sem=b_send.at[i],
            recv_sem=b_recv.at[i],
            device_id={"fs": other},
            device_id_type=MESH,
        )

    load_down.wait()
    down.all_along(f, start)
    for d in range(1, n_tp):
        a_copy(d).start()
    for load in loads:
        load.wait()
    load_hid.wait()

    @pl.when(jnp.logical_not(is_host))
    def _():
        hosted.all_along(f, start)

    def first_half(k, carry):
        src = source(k)

        down.take(src)

        @pl.when((k == 2 * n_fs - 2) & is_host)
        def _():
            hosted.all_along(f, start)

        @pl.when(k == 2)
        def _():
            for d in range(1, n_tp):
                a_copy(d).wait_recv()

        done = source(k - 2)

        @pl.when((k >= 2) & valid(done))
        def _():
            down.take_across(done)
            part[done] = jnp.dot(
                spread[...], down_all[done], preferred_element_type=jnp.float32
            ).astype(jnp.bfloat16)
            for d in range(1, n_tp):
                r_copy(done, d).start()

        return carry

    lax.fori_loop(1, 2 * n_fs + 1, first_half, 0)

    for src in range(n_fs):
        for d in range(1, n_tp):
            r_copy(src, d).wait_recv()
    pieces = []
    for src in range(n_fs):
        total = part[src, own_rows(t)].astype(jnp.float32)
        for d in range(1, n_tp):
            total = total + red[d, src].astype(jnp.float32)
        pieces.append(total)
    branch = jnp.concatenate(pieces, axis=1)
    first = layer_norm(
        jnp.sqrt(2.0) * res_ref[...].astype(jnp.float32) + 0.5 * branch,
        gain_ref[0:1],
        shift_ref[0:1],
    )
    mixed = layer_norm(
        jnp.sqrt(2.0) * first + mix_ref[...].astype(jnp.float32), gain_ref[1:2], shift_ref[1:2]
    ).astype(jnp.bfloat16)
    mixed_all[0, own_rows(t)] = mixed
    mixed_ref[...] = mixed

    @pl.when(jnp.logical_not(is_host))
    def _():
        g_copy().start()

    m_out(0)

    @pl.when(jnp.logical_not(is_host))
    def _():
        each.all_along(f, start)

    def take_hosted(k, carry):
        hosted.take(source(k))
        return carry

    lax.fori_loop(1, 2 * n_fs - 1, take_hosted, 0)

    @pl.when(is_host)
    def _():
        each.all_along(f, start)

    m_relay(0)

    @pl.when(is_host)
    def _():
        g_copy().wait_recv()
        m_out(1)

    def take_each(k, carry):
        each.take(source(k))
        return carry

    lax.fori_loop(1, 3, take_each, 0)
    m_rest(0)

    def products(whose, span, gather, refs, total):
        total[...] = jnp.zeros_like(total)

        def add(k, carry):
            src = source(k)

            @pl.when(valid(src))
            def _():
                if gather is not None:
                    gather.take_across(src)
                here = pl.ds(pl.multiple_of(src * depth, depth), depth)
                for mat in range(2):
                    total[mat] += jnp.dot(
                        mixed_all[whose, span, here],
                        refs[src, mat],
                        preferred_element_type=jnp.float32,
                    )

            return carry

        lax.fori_loop(0, 2 * n_fs - 1, add, 0)
        gate = total[0]
        return (gate / (1.0 + jnp.exp(-gate)) * total[1]).astype(jnp.bfloat16)

    everything = pl.ds(0, n_tp * rows)

    @pl.when(is_host)
    def _():
        m_relay(1)
        out_ref[:, pl.ds(0, shared)] = products(0, everything, hosted, host_all, host_acc)

    lax.fori_loop(3, 2 * n_fs - 1, take_each, 0)

    @pl.when(is_host)
    def _():
        m_rest(1)

        def serve(i, carry):
            back[tile_rows(i)] = products(
                1, tile_rows(i), None, host_all, host_acc.at[:, pl.ds(0, tile)]
            )
            b_copy(i).start()
            return carry

        lax.fori_loop(0, tiles, serve, 0)

    out_ref[:, pl.ds(shared, width - shared)] = products(0, everything, each, each_all, each_acc)

    @pl.when(is_host)
    def _():
        for i in range(tiles):
            b_copy(i).wait_send()
        m_drain(1)

    @pl.when(jnp.logical_not(is_host))
    def _():
        g_copy().wait_send()
        for i in range(tiles):
            b_copy(i).wait_recv()

    m_drain(0)
    for d in range(1, n_tp):
        a_copy(d).wait_send()
        for src in range(n_fs):
            r_copy(src, d).wait_send()

    def drain(src, carry):
        for gather in (down, hosted, each):
            gather.drain(src)
        return carry

    lax.fori_loop(0, n_fs, drain, 0)


def on_device(
    sizes,
    residual_in,
    hidden_first,
    down_weight,
    mixer_out,
    norm_gain,
    norm_shift,
    gate_weight,
    up_weight,
):
    n_grp, n_fs, n_tp = sizes
    rows, model = residual_in.shape
    depth, width = gate_weight.shape
    cols = down_weight.shape[1]
    sub = 1
    if depth % (n_grp * 2 * 32) == 0 and down_weight.shape[0] % (n_grp * 2 * 32) == 0:
        sub = 2
    chunks = n_grp * sub
    each = max(1, width * 3 // (11 * 128)) * 128
    shared = (width - each) // 128 * 128
    each = width - shared
    if width % 128:
        hidden_first = hidden_first.reshape(rows, n_tp, width).transpose(1, 0, 2)
    vmem = pl.BlockSpec(memory_space=pltpu.VMEM)
    anywhere = pl.BlockSpec(memory_space=pl.ANY)
    dma = pltpu.SemaphoreType.DMA
    tokens = rows * n_tp
    return pl.pallas_call(
        functools.partial(kernel, (n_grp, n_fs, n_tp, sub)),
        out_shape=(
            jax.ShapeDtypeStruct((rows, model), jnp.bfloat16),
            jax.ShapeDtypeStruct((tokens, width), jnp.bfloat16),
        ),
        in_specs=[vmem, anywhere, anywhere, vmem, vmem, vmem, anywhere, anywhere],
        out_specs=(vmem, vmem),
        scratch_shapes=[
            pltpu.VMEM((n_fs,) + down_weight.shape, jnp.bfloat16),
            pltpu.VMEM((n_fs, 2, depth, shared), jnp.bfloat16),
            pltpu.VMEM((n_fs, 2, depth, each), jnp.bfloat16),
            pltpu.VMEM((tokens, width), jnp.bfloat16),
            pltpu.VMEM((n_fs, tokens, cols), jnp.bfloat16),
            pltpu.VMEM((n_tp, n_fs, rows, cols), jnp.bfloat16),
            pltpu.VMEM((2, tokens, model), jnp.bfloat16),
            pltpu.VMEM((2, tokens, shared), jnp.float32),
            pltpu.VMEM((2, tokens, each), jnp.float32),
            pltpu.VMEM((tokens, shared), jnp.bfloat16),
            dma((6,)),
            dma((n_fs, 1 + n_grp, chunks)),
            dma((n_fs, chunks)),
            dma((2 * n_fs, 1 + n_grp, chunks)),
            dma((2 * n_fs, chunks)),
            dma((2 * n_fs, 1 + n_grp, chunks)),
            dma((2 * n_fs, chunks)),
            dma((n_tp,)),
            dma((n_tp,)),
            dma((n_tp, n_fs)),
            dma((n_tp, n_fs)),
            dma((2, n_tp, n_tp // 2)),
            dma((2, n_tp)),
            dma((1,)),
            dma((1,)),
            dma((2,)),
            dma((2,)),
        ],
        compiler_params=pltpu.CompilerParams(
            collective_id=0, has_side_effects=True, vmem_limit_bytes=60 * 1024 * 1024
        ),
        name="half_steps",
    )(
        residual_in,
        hidden_first,
        down_weight,
        mixer_out,
        norm_gain,
        norm_shift,
        gate_weight,
        up_weight,
    )


def solution(mesh):
    sizes = tuple(mesh.shape[axis] for axis in ("grp", "fs", "tp"))
    in_specs = (
        P(("grp", "fs", "tp"), None),
        P(("grp", "fs", "tp"), None),
        P("tp", "fs"),
        P(("grp", "fs", "tp"), None),
        P(),
        P(),
        P("fs", "tp"),
        P("fs", "tp"),
    )
    out_specs = (P(("grp", "fs", "tp"), None), P(("grp", "fs"), "tp"))
    return jax.shard_map(
        functools.partial(on_device, sizes),
        mesh=mesh,
        in_specs=in_specs,
        out_specs=out_specs,
        check_vma=False,
    )
```
